32 devices in a mesh: kv: 16 (over z, y, x), tp: 2 (over core).
Axes of the slice: x: 2, y: 2, z: 4, core: 2. Of those that a mesh axis runs over, the one named last changes fastest.
Arguments:
- hidden_in: bfloat16 [8, 1024], P(None, 'tp'), may hold values from -18 to 18, as said below
- input_gain: float32 [1024], P('tp'), may hold values from 0.1 to 1.9
- down_query: bfloat16 [1024, 256], P('tp'), may hold values from -0.1875 to 0.1875
- down_latent: bfloat16 [1024, 256], P('tp'), may hold values from -0.1875 to 0.1875
- down_rope: bfloat16 [1024, 64], P('tp'), may hold values from -0.1875 to 0.1875
- query_gain: float32 [256], replicated, may hold values from 0.1 to 1.9
- latent_gain: float32 [256], replicated, may hold values from 0.1 to 1.9
- up_query: bfloat16 [256, 8, 128], P(None, 'tp'), may hold values from -0.375 to 0.375
- up_rope: bfloat16 [256, 8, 64], P(None, 'tp'), may hold values from -0.375 to 0.375
- key_up: bfloat16 [256, 8, 128], P(None, 'tp'), may hold values from -0.375 to 0.375
- value_up: bfloat16 [256, 8, 128], P(None, 'tp'), may hold values from -0.375 to 0.375
- out_proj: bfloat16 [1024, 1024], P('tp', 'kv'), may hold values from -2 to 2, as said below
- output_gain: float32 [1024], P('kv'), may hold values from 0.1 to 1.9
- latent_cache: bfloat16 [8, 4096, 256], P(None, ('kv', 'tp')), may hold values from -6 to 6
- rope_cache: bfloat16 [8, 4096, 64], P(None, ('kv', 'tp')), may hold values from -6 to 6
- lengths: int32 [8], replicated, may hold values from 1 to 4096, as said below
Outputs:
- mixed: bfloat16 [8, 1024], P(None, 'kv')
The draws below stay inside these ranges and needn't reach their ends.
Inputs may be any that keep to these rules, and one draw needn't show every extreme that they name: Each length lies between 1 and 4096; in every draw some sequence has exactly 4096 and some exactly 1; lengths are heavily skewed toward short ones. `hidden_in`: activations whose size differs strongly between blocks of 64 features, by sequence. `out_proj`: output projection whose columns differ strongly in size.
All inputs are finite; a program needn't handle non-finite values.
Results may differ from the reference program's by a relative error of at most 0.015.
Values may be sent and summed in bfloat16 or wider, within the bound.
A program may use at most 128 MiB of HBM per device.

```python
import math
import jax
import jax.numpy as jnp
from jax import lax

D = 1024
H = 8
DN = 128
DR = 64
DV = 128
QR = 256
KR = 256
SEQS = 8
LEN = 4096


def draw_lengths(key, part):
    subkeys = jax.random.split(key, 3)
    drawn = jax.random.randint(subkeys[0], (SEQS,), 1, LEN + 1)
    shifts = jax.random.randint(subkeys[1], (SEQS,), 0, LEN.bit_length())
    result = jnp.maximum(jnp.right_shift(drawn, shifts), 1)
    chosen = jax.random.randint(subkeys[2], (), 0, SEQS)
    result = result.at[chosen].set(LEN)
    result = result.at[(chosen + 1) % SEQS].set(1)
    return result.astype(jnp.int32)


def draw_hidden_in(key, part):
    subkeys = jax.random.split(jax.random.fold_in(key, 11), 2)
    blocks = D // 64
    base = jnp.clip(jax.random.normal(subkeys[0], (SEQS, blocks, 64), jnp.float32), -4.0, 4.0)
    spread = jnp.exp(jax.random.uniform(subkeys[1], (SEQS, blocks, 1), jnp.float32, -1.5, 1.5))
    return (base * spread).reshape(SEQS, D).astype(jnp.bfloat16)


def draw_out_proj(key, part):
    subkeys = jax.random.split(jax.random.fold_in(key, 23), 2)
    base = jnp.clip(jax.random.normal(subkeys[0], (H * DV, D), jnp.float32), -4.0, 4.0)
    spread = jnp.exp(jax.random.uniform(subkeys[1], (1, D), jnp.float32, -1.5, 1.5))
    return (base * spread / jnp.sqrt(jnp.float32(H * DV))).astype(jnp.bfloat16)


def shard_levels(own_key, extent, cuts, least, high):
    level, own = 1.0, jax.random.fold_in(own_key, 6)
    for dim, parts in cuts:
        steps = jnp.exp(jax.random.uniform(jax.random.fold_in(own, dim), (parts,), jnp.float32, least / len(cuts), high / len(cuts)))
        level = level * jnp.repeat(steps, extent[dim] // parts).reshape([-1 if axis == dim else 1 for axis in range(len(extent))])
    return level


def centred(rng, dims, width, bound, pieces=(), kind=jnp.bfloat16):
    loudness = shard_levels(rng, dims, pieces, -0.22, 0.18) if pieces else 1.0
    values = jax.random.normal(rng, dims, jnp.float32) * width * loudness
    return jnp.minimum(jnp.maximum(values, -bound), bound).astype(kind)


def setup_inputs(seed: int = 0) -> dict:
    seeds = jax.random.split(jax.random.key(seed), 17)
    return {
        "hidden_in": draw_hidden_in(jax.random.fold_in(seeds[16], 71), 0),
        "input_gain": jnp.clip(1.0 + 0.18 * jax.random.normal(seeds[1], (D,), jnp.float32), 0.1, 1.9),
        "down_query": centred(seeds[2], (D, QR), D ** -0.5, 0.1875, ((0, 2),)),
        "down_latent": centred(seeds[3], (D, KR), D ** -0.5, 0.1875, ((0, 2),)),
        "down_rope": centred(seeds[4], (D, DR), D ** -0.5, 0.1875, ((0, 2),)),
        "query_gain": jnp.clip(1.0 + 0.18 * jax.random.normal(seeds[5], (QR,), jnp.float32), 0.1, 1.9),
        "latent_gain": jnp.clip(1.0 + 0.18 * jax.random.normal(seeds[6], (KR,), jnp.float32), 0.1, 1.9),
        "up_query": centred(seeds[7], (QR, H, DN), QR ** -0.5, 0.375, ((1, 2),)),
        "up_rope": centred(seeds[8], (QR, H, DR), QR ** -0.5, 0.375, ((1, 2),)),
        "key_up": centred(seeds[9], (KR, H, DN), KR ** -0.5, 0.375, ((1, 2),)),
        "value_up": centred(seeds[10], (KR, H, DV), KR ** -0.5, 0.375, ((1, 2),)),
        "out_proj": draw_out_proj(jax.random.fold_in(seeds[16], 71), 0),
        "output_gain": jnp.clip(1.0 + 0.18 * jax.random.normal(seeds[12], (D,), jnp.float32), 0.1, 1.9),
        "latent_cache": centred(seeds[13], (SEQS, LEN, KR), 1.0, 6.0, ((1, 32),)),
        "rope_cache": centred(seeds[14], (SEQS, LEN, DR), 1.0, 6.0, ((1, 32),)),
        "lengths": draw_lengths(jax.random.fold_in(seeds[16], 71), 0),
    }


THETA = 10000.0
EPSILON = 1e-06

def rotate(values, angles):
    half_width = values.shape[-1] // 2
    first_half = values[..., :half_width]
    second_half = values[..., half_width:]
    cosine = jnp.cos(angles)
    sine_part = jnp.sin(angles)
    return jnp.concatenate([first_half * cosine - second_half * sine_part, second_half * cosine + first_half * sine_part], axis=-1)

def angles_for(positions, rot_width):
    inverse = 1.0 / THETA ** (jnp.arange(0, rot_width, 2, dtype=jnp.float32) / rot_width)
    return positions[:, None] * inverse[None, :]

def normed(values, gain_row):
    return values * lax.rsqrt(lax.optimization_barrier(jnp.mean(values * values, axis=-1, keepdims=True)) + EPSILON) * gain_row.astype(jnp.float32)

def widen(values):
    return values.astype(jnp.float32)

def settle(values):
    return lax.optimization_barrier(values.astype(jnp.bfloat16))

def reference(hidden_in, input_gain, down_query, down_latent, down_rope, query_gain, latent_gain, up_query, up_rope, key_up, value_up, out_proj, output_gain, latent_cache, rope_cache, lengths):
    floats = widen(hidden_in)
    inv_rms = lax.rsqrt(lax.optimization_barrier(jnp.mean(floats * floats, axis=1, keepdims=True)) + EPSILON)
    scaled = (floats * widen(input_gain)).astype(jnp.bfloat16)
    query_low = jnp.dot(scaled, down_query, preferred_element_type=jnp.float32) * inv_rms
    latent_low = jnp.dot(scaled, down_latent, preferred_element_type=jnp.float32) * inv_rms
    rope_low = jnp.dot(scaled, down_rope, preferred_element_type=jnp.float32) * inv_rms
    positions = lengths.astype(jnp.float32)
    query_normed = settle(normed(query_low, query_gain))
    query_nope = settle(jnp.einsum('bq,qhd->bhd', widen(query_normed), widen(up_query)))
    query_rope = jnp.einsum('bq,qhr->bhr', widen(query_normed), widen(up_rope))
    query_rope = settle(rotate(query_rope, angles_for(positions, DR)[:, None, :]))
    latent_query = settle(jnp.einsum('bhd,chd->bhc', widen(query_nope), widen(key_up)))
    latent_new = settle(normed(latent_low, latent_gain))
    rope_new = settle(rotate(rope_low, angles_for(positions, DR)))
    factor = 1.0 / math.sqrt(DN + DR)
    places = jnp.arange(LEN, dtype=jnp.int32)

    def one_sequence(inputs):
        seq_query, seq_rope, latents, rotated, fresh_latent, fresh_rope, length = inputs
        scores = (jnp.einsum('hc,pc->hp', widen(seq_query), widen(latents)) + jnp.einsum('hr,pr->hp', widen(seq_rope), widen(rotated))) * factor
        usable = places < length
        scores = jnp.where(usable[None, :], scores, -1e+30)
        new_score = (lax.optimization_barrier(jnp.sum(widen(seq_query) * widen(fresh_latent)[None, :], axis=-1)) + lax.optimization_barrier(jnp.sum(widen(seq_rope) * widen(fresh_rope)[None, :], axis=-1))) * factor
        highest = jnp.maximum(lax.optimization_barrier(jnp.max(scores, axis=-1)), new_score)
        weights = jnp.where(usable[None, :], jnp.exp(scores - highest[:, None]), 0.0)
        fresh_weight = jnp.exp(new_score - highest)
        total_mass = lax.optimization_barrier(jnp.sum(weights, axis=-1)) + fresh_weight
        summed = jnp.einsum('hp,pc->hc', widen(settle(weights)), widen(latents)) + fresh_weight[:, None] * widen(fresh_latent)[None, :]
        return summed / total_mass[:, None]
    attended = lax.map(one_sequence, (latent_query, query_rope, latent_cache, rope_cache, latent_new, rope_new, lengths))
    attended = settle(attended)
    values_out = settle(jnp.einsum('bhc,chv->bhv', widen(attended), widen(value_up)))
    flattened = values_out.reshape(values_out.shape[0], H * DV)
    out_full = jnp.dot(flattened, out_proj, preferred_element_type=jnp.float32)
    out_rms = lax.rsqrt(lax.optimization_barrier(jnp.mean(out_full * out_full, axis=1, keepdims=True)) + EPSILON)
    return (out_full * out_rms * widen(output_gain)).astype(jnp.bfloat16)
```

```python
import functools
import math

import jax
import jax.numpy as jnp
import numpy as np
from jax import lax
from jax.experimental import pallas as pl
from jax.experimental.pallas import tpu as pltpu
from jax.sharding import PartitionSpec as P

THETA = 10000.0
EPSILON = 1e-06
MESH = pl.DeviceIdType.MESH
F32 = jnp.float32
BF16 = jnp.bfloat16
NT = (((1,), (1,)), ((), ()))


def iota(shape, dim):
    return lax.broadcasted_iota(jnp.int32, shape, dim)


def dot(a, b):
    return jnp.dot(a, b, preferred_element_type=F32)


def dot_nt(a, b):
    return lax.dot_general(a, b, NT, preferred_element_type=F32)


def sin_cos(x):
    turns = jnp.floor(x * (1.0 / (2 * math.pi)) + 0.5)
    r = (x - turns * 6.28125) - turns * (2 * math.pi - 6.28125)
    r2 = r * r
    s = jnp.full_like(x, 1.0)
    for n in (15, 13, 11, 9, 7, 5, 3):
        s = 1.0 - s * r2 * (1.0 / (n * (n - 1)))
    c = jnp.full_like(x, 1.0)
    for n in (18, 16, 14, 12, 10, 8, 6, 4, 2):
        c = 1.0 - c * r2 * (1.0 / (n * (n - 1)))
    return s * r, c


def turn(v, cosine, sine):
    half = v.shape[-1] // 2
    swapped = jnp.concatenate([-v[:, half:], v[:, :half]], axis=1)
    return v * cosine + swapped * sine


def normed(v, gain):
    return v * lax.rsqrt(jnp.mean(v * v, axis=-1, keepdims=True) + EPSILON) * gain


def kernel(
    K,
    T,
    lengths,
    inverse,
    hidden_h,
    gain_h,
    dq_h,
    dl_h,
    dr_h,
    qg_h,
    lg_h,
    uq_h,
    ur_h,
    ku_h,
    vu_h,
    op_h,
    og_h,
    lat_h,
    rope_h,
    out,
    hidden,
    gain,
    dq,
    dl,
    dr,
    qg,
    lg,
    uq,
    ur,
    ku,
    vu,
    og,
    lat,
    rope,
    rx1,
    rx2,
    rxp,
    tx3,
    rx3,
    tx4,
    rx4,
    rx6,
    spread,
    load_sem,
    s1,
    r1,
    s2,
    r2,
    sp,
    rp,
    s3,
    r3,
    s4,
    r4,
    s6,
    r6,
):
    N = K * T
    B = hidden.shape[0]
    width = hidden.shape[1] * T
    QR = dq.shape[1]
    KR = dl.shape[1]
    DR = dr.shape[0]
    Hd = uq.shape[0] // QR
    H = Hd * T
    DN = uq.shape[1]
    span = lat.shape[1]
    rows = rx3.shape[1]
    owners = tx3.shape[0]
    k = lax.axis_index("kv")
    t = lax.axis_index("tp")
    me = k * T + t
    factor = 1.0 / math.sqrt(DN + DR)

    def place(d):
        return (lax.div(d, T), lax.rem(d, T))

    def slot_of(d):
        first = lax.div(d, T) * rows
        return lax.div(lax.div(first, Hd) * H + lax.rem(d, T) * Hd + lax.rem(first, Hd), rows)

    everyone_owns = owners == N

    def if_owner(d, fn):
        if everyone_owns:
            fn()
        else:
            pl.when(lax.div(d, T) * T * rows < B * H)(fn)

    barrier = pltpu.get_barrier_semaphore()

    def greet(i, carry):
        pl.semaphore_signal(barrier, inc=1, device_id=place(lax.rem(me + i, N)), device_id_type=MESH)
        return carry

    lax.fori_loop(1, N, greet, 0)

    pairs = (
        (hidden_h, hidden), (gain_h, gain), (dq_h, dq), (dl_h, dl), (dr_h, dr),
        (uq_h, uq), (ur_h, ur), (ku_h, ku), (qg_h, qg), (lg_h, lg),
        (op_h, rxp.at[t]), (lat_h, lat), (rope_h, rope), (vu_h, vu), (og_h, og),
    )
    loads = [pltpu.make_async_copy(a, b, load_sem.at[i]) for i, (a, b) in enumerate(pairs)]
    for load in loads:
        load.start()

    spread[...] = jnp.where(
        lax.div(iota((QR, QR * Hd), 1), Hd) == iota((QR, QR * Hd), 0), 1.0, 0.0
    ).astype(BF16)
    own_rows = iota((B * H, QR * Hd), 0)
    own_mask = (lax.rem(own_rows, H) - t * Hd) == lax.rem(iota((B * H, QR * Hd), 1), Hd)

    def angles(n, per):
        row = lax.div(iota((n, DR), 0), per)
        position = jnp.zeros((n, DR), F32)
        for b in range(B):
            position = jnp.where(row == b, lengths[b].astype(F32), position)
        return sin_cos(position * inverse[...])

    sine8, cosine8 = angles(B, 1)
    sine_all, cosine_all = angles(B * H, H)

    for load in loads[:5]:
        load.wait()
    floats = hidden[...].astype(F32)
    scaled = (floats * gain[...]).astype(BF16)
    low = rx1.at[t]
    low[:, :QR] = dot(scaled, dq[...])
    low[:, QR : QR + KR] = dot(scaled, dl[...])
    low[:, QR + KR : QR + KR + DR] = dot_nt(scaled, dr[...])
    low[:, QR + KR + DR :] = jnp.broadcast_to(
        jnp.sum(floats * floats, axis=1, keepdims=True), (B, rx1.shape[2] - QR - KR - DR)
    )
    pl.semaphore_wait(barrier, N - 1)

    def swap(buffer, send, recv):
        copies = []
        for i in range(1, T):
            peer = lax.rem(t + i, T)
            copies.append(
                pltpu.make_async_remote_copy(
                    src_ref=buffer.at[t],
                    dst_ref=buffer.at[t],
                    send_sem=send.at[i],
                    recv_sem=recv.at[i],
                    device_id=(k, peer),
                    device_id_type=MESH,
                )
            )
        for copy in copies:
            copy.start()
        return copies

    copies1 = swap(rx1, s1, r1)
    for load in loads[5:]:
        load.wait()
    for copy in copies1:
        copy.wait()
    total = rx1[0]
    for i in range(1, T):
        total = total + rx1[i]
    inv_rms = lax.rsqrt(total[:, QR + KR + DR : QR + KR + DR + 1] / width + EPSILON)
    total = total * inv_rms
    query_normed = normed(total[:, :QR], qg[...]).astype(BF16)
    latent_new = normed(total[:, QR : QR + KR], lg[...]).astype(BF16).astype(F32)
    rope_new = turn(total[:, QR + KR : QR + KR + DR], cosine8, sine8).astype(BF16).astype(F32)

    wide = dot(query_normed, spread[...])
    wide = jnp.concatenate(
        [jnp.broadcast_to(wide[b : b + 1, :], (H, QR * Hd)) for b in range(B)], axis=0
    )
    wide = jnp.where(own_mask, wide, 0.0).astype(BF16)
    query_nope = dot(wide, uq[...]).astype(BF16)
    roped = dot_nt(query_normed, ur[...])
    roped = jnp.concatenate(
        [jnp.broadcast_to(roped[b : b + 1, :], (H, Hd * DR)) for b in range(B)], axis=0
    )
    head = lax.rem(iota((B * H, DR), 0), H) - t * Hd
    query_rope = jnp.zeros((B * H, DR), F32)
    for h in range(Hd):
        query_rope = jnp.where(head == h, roped[:, h * DR : (h + 1) * DR], query_rope)
    query_rope = turn(query_rope, cosine_all, sine_all)
    tall = jnp.where(own_mask, dot_nt(query_nope, ku[...]), 0.0).astype(BF16)
    queries = rx2.at[t]
    queries[:, :KR] = dot_nt(tall, spread[...]).astype(BF16)
    queries[:, KR : KR + DR] = query_rope.astype(BF16)
    queries[:, KR + DR :] = jnp.zeros((B * H, rx2.shape[2] - KR - DR), BF16)
    copies2 = swap(rx2, s2, r2)
    copies_p = swap(rxp, sp, rp)
    for copy in copies2:
        copy.wait()
    query = rx2[0].astype(F32)
    for i in range(1, T):
        query = query + rx2[i].astype(F32)

    offset = me * span
    lane = iota((H, span), 1) + offset
    mark = iota((H, 128), 1)
    first = me == 0
    for b in range(B):
        q = query[b * H : (b + 1) * H]
        qb = q.astype(BF16)
        usable = lane < lengths[b]
        scores = (
            dot_nt(qb[:, :KR], lat[b]) + dot(qb[:, KR : KR + DR], rope[b])
        ) * factor
        scores = jnp.where(usable, scores, -1e30)
        new_score = (
            jnp.sum(q[:, :KR] * latent_new[b : b + 1], axis=1, keepdims=True)
            + jnp.sum(q[:, KR : KR + DR] * rope_new[b : b + 1], axis=1, keepdims=True)
        ) * factor
        new_score = jnp.where(first, new_score, -1e30)
        top = jnp.maximum(jnp.max(scores, axis=1, keepdims=True), new_score)
        weights = jnp.where(usable, jnp.exp(scores - top), 0.0)
        fresh = jnp.where(first, jnp.exp(new_score - top), 0.0)
        mass = jnp.sum(weights, axis=1, keepdims=True) + fresh
        summed = dot(weights.astype(BF16), lat[b]) + fresh * latent_new[b : b + 1]
        high = top.astype(BF16).astype(F32)
        middle = (top - high).astype(BF16).astype(F32)
        small = ((top - high) - middle).astype(BF16).astype(F32)
        mass_high = mass.astype(BF16).astype(F32)
        tail = jnp.where(
            mark == 0,
            high,
            jnp.where(
                mark == 1,
                middle,
                jnp.where(mark == 2, small, jnp.where(mark == 3, mass_high, mass - mass_high)),
            ),
        )
        block = jnp.concatenate([summed, tail], axis=1).astype(BF16)
        for j in range(H // rows):
            tx3[b * (H // rows) + j] = block[j * rows : (j + 1) * rows]

    def part(d):
        return pltpu.make_async_remote_copy(
            src_ref=tx3.at[slot_of(d)],
            dst_ref=rx3.at[me],
            send_sem=s3,
            recv_sem=r3,
            device_id=place(d),
            device_id_type=MESH,
        )

    def send3(i, carry):
        d = lax.rem(me + i, N)
        if_owner(d, part(d).start)
        return carry

    lax.fori_loop(1, N, send3, 0)

    mine = slot_of(me)

    def values(d):
        return pltpu.make_async_remote_copy(
            src_ref=tx4,
            dst_ref=rx4.at[mine],
            send_sem=s4,
            recv_sem=r4,
            device_id=place(d),
            device_id_type=MESH,
        )

    def own():
        rx3[me] = tx3[mine]
        pltpu.make_async_copy(rx3.at[pl.ds(0, N - 1)], rx3.at[pl.ds(0, N - 1)], r3).wait()
        parts = rx3[...].astype(F32)
        tail = parts[:, :, KR : KR + 128]
        top = tail[:, :, 0:1] + tail[:, :, 1:2] + tail[:, :, 2:3]
        highest = jnp.max(top, axis=0, keepdims=True)
        scale = jnp.exp(top - highest)
        mass = jnp.sum((tail[:, :, 3:4] + tail[:, :, 4:5]) * scale, axis=0)
        attended = jnp.sum(parts[:, :, :KR] * scale, axis=0) / mass
        attended = jnp.concatenate([attended, jnp.zeros((8 - rows, KR), F32)], axis=0)
        wide = dot(attended.astype(BF16), spread[...])
        head = lax.rem(k * rows + iota((8, KR * Hd), 0), Hd)
        wide = jnp.where(head == lax.rem(iota((8, KR * Hd), 1), Hd), wide, 0.0).astype(BF16)
        value = dot(wide, vu[...])[:rows].astype(BF16)
        tx4[...] = value
        rx4[mine] = value

        def send4(i, carry):
            values(lax.rem(me + i, N)).start()
            return carry

        lax.fori_loop(1, N, send4, 0)

    if_owner(me, own)
    for copy in copies_p:
        copy.wait()

    def arrived(n):
        pltpu.make_async_copy(rx4.at[pl.ds(0, n)], rx4.at[pl.ds(0, n)], r4).wait()

    if everyone_owns:
        arrived(owners - 1)
    else:
        owner = k * T * rows < B * H
        pl.when(owner)(lambda: arrived(owners - 1))
        pl.when(jnp.logical_not(owner))(lambda: arrived(owners))

    gathered = rx4[...].astype(F32).reshape(B, H, rx4.shape[2]).astype(BF16)
    out_cols = jnp.zeros(out.shape, F32)
    for i in range(T):
        flat = jnp.concatenate([gathered[:, i * Hd + h, :] for h in range(Hd)], axis=1)
        out_cols = out_cols + dot_nt(flat, rxp[i])
    squares = jnp.sum(out_cols * out_cols, axis=1, keepdims=True)
    diagonal = iota((B, 128), 0) == iota((B, 128), 1)
    rx6[k] = jnp.sum(jnp.where(diagonal, squares, 0.0), axis=0, keepdims=True)

    def norm_part(i):
        return pltpu.make_async_remote_copy(
            src_ref=rx6.at[k],
            dst_ref=rx6.at[k],
            send_sem=s6,
            recv_sem=r6,
            device_id=(lax.rem(k + i, K), t),
            device_id_type=MESH,
        )

    def send6(i, carry):
        norm_part(i).start()
        return carry

    lax.fori_loop(1, K, send6, 0)

    def sent3(i, carry):
        d = lax.rem(me + i, N)
        if_owner(d, part(d).wait_send)
        return carry

    def sent4(i, carry):
        values(lax.rem(me + i, N)).wait_send()
        return carry

    lax.fori_loop(1, N, sent3, 0)
    def left4():
        lax.fori_loop(1, N, sent4, 0)

    if_owner(me, left4)

    pltpu.make_async_copy(rx6.at[pl.ds(0, K - 1)], rx6.at[pl.ds(0, K - 1)], r6).wait()
    total = jnp.sum(rx6[...], axis=0)
    squares = jnp.sum(
        jnp.where(diagonal, jnp.broadcast_to(total, (B, 128)), 0.0), axis=1, keepdims=True
    )
    out[...] = (out_cols * lax.rsqrt(squares / width + EPSILON) * og[...]).astype(BF16)

    def sent6(i, carry):
        norm_part(i).wait_send()
        return carry

    lax.fori_loop(1, K, sent6, 0)


def shards(
    K, T, hidden_in, input_gain, down_query, down_latent, down_rope, query_gain, latent_gain,
    up_query, up_rope, key_up, value_up, out_proj, output_gain, latent_cache, rope_cache, lengths,
):
    B = hidden_in.shape[0]
    QR, Hd, DN = up_query.shape
    KR, DR, DV = key_up.shape[0], up_rope.shape[2], value_up.shape[2]
    H, N = Hd * T, K * T
    rows = max(1, B * Hd // K)
    owners = B * H // rows
    steps = np.arange(0, DR, 2, dtype=np.float64) / DR
    inverse = np.tile((1.0 / THETA**steps).astype(np.float32), 2)[None, :]
    flat = lambda w: w.reshape(w.shape[0] * w.shape[1], w.shape[2])
    row = lambda v: v.reshape(1, v.shape[0])
    arrays = (
        hidden_in, row(input_gain), down_query, down_latent, down_rope.T, row(query_gain),
        row(latent_gain), flat(up_query), flat(up_rope.transpose(1, 2, 0)), flat(key_up),
        flat(value_up), out_proj.T, row(output_gain), latent_cache,
        rope_cache.transpose(0, 2, 1),
    )
    vm = lambda a: pltpu.VMEM(a.shape, a.dtype)
    local = [vm(a) for i, a in enumerate(arrays) if i != 11]
    low = -(-(QR + KR + DR + 1) // 128) * 128
    wide = -(-(KR + DR) // 128) * 128
    dma = pltpu.SemaphoreType.DMA
    scratch = local + [
        pltpu.VMEM((T, B, low), F32),
        pltpu.VMEM((T, B * H, wide), BF16),
        pltpu.VMEM((T,) + out_proj.shape[::-1], BF16),
        pltpu.VMEM((owners, rows, KR + 128), BF16),
        pltpu.VMEM((N, rows, KR + 128), BF16),
        pltpu.VMEM((rows, DV), BF16),
        pltpu.VMEM((owners, rows, DV), BF16),
        pltpu.VMEM((K, 1, 128), F32),
        pltpu.VMEM((QR, QR * Hd), BF16),
        dma((len(arrays),)),
        dma((T,)), dma((T,)), dma((T,)), dma((T,)), dma((T,)), dma((T,)),
        dma, dma, dma, dma, dma, dma,
    ]
    return pl.pallas_call(
        functools.partial(kernel, K, T),
        out_shape=jax.ShapeDtypeStruct((B, out_proj.shape[1]), BF16),
        in_specs=[
            pl.BlockSpec(memory_space=pltpu.SMEM),
            pl.BlockSpec(memory_space=pltpu.VMEM),
        ]
        + [pl.BlockSpec(memory_space=pl.ANY)] * len(arrays),
        out_specs=pl.BlockSpec(memory_space=pltpu.VMEM),
        scratch_shapes=scratch,
        compiler_params=pltpu.CompilerParams(collective_id=0, has_side_effects=True),
    )(lengths, jnp.asarray(inverse), *arrays)


def solution(mesh):
    in_specs = (
        P(None, "tp"),
        P("tp"),
        P("tp", None),
        P("tp", None),
        P("tp", None),
        P(),
        P(),
        P(None, "tp", None),
        P(None, "tp", None),
        P(None, "tp", None),
        P(None, "tp", None),
        P("tp", "kv"),
        P("kv"),
        P(None, ("kv", "tp"), None),
        P(None, ("kv", "tp"), None),
        P(),
    )
    body = functools.partial(shards, mesh.shape["kv"], mesh.shape["tp"])
    return jax.shard_map(body, mesh=mesh, in_specs=in_specs, out_specs=P(None, "kv"), check_vma=False)
```

```python
import functools
import math

import jax
import jax.numpy as jnp
import numpy as np
from jax import lax
from jax.experimental import pallas as pl
from jax.experimental.pallas import tpu as pltpu
from jax.sharding import PartitionSpec as P

THETA = 10000.0
EPSILON = 1e-06
MESH = pl.DeviceIdType.MESH
F32 = jnp.float32
BF16 = jnp.bfloat16
NT = (((1,), (1,)), ((), ()))


def iota(shape, dim):
    return lax.broadcasted_iota(jnp.int32, shape, dim)


def dot(a, b):
    return jnp.dot(a, b, preferred_element_type=F32)


def dot_nt(a, b):
    return lax.dot_general(a, b, NT, preferred_element_type=F32)


def sin_cos(x):
    turns = jnp.floor(x * (1.0 / (2 * math.pi)) + 0.5)
    r = (x - turns * 6.28125) - turns * (2 * math.pi - 6.28125)
    r2 = r * r
    s = jnp.full_like(x, 1.0)
    for n in (15, 13, 11, 9, 7, 5, 3):
        s = 1.0 - s * r2 * (1.0 / (n * (n - 1)))
    c = jnp.full_like(x, 1.0)
    for n in (18, 16, 14, 12, 10, 8, 6, 4, 2):
        c = 1.0 - c * r2 * (1.0 / (n * (n - 1)))
    return s * r, c


def turn(v, cosine, sine):
    half = v.shape[-1] // 2
    swapped = jnp.concatenate([-v[:, half:], v[:, :half]], axis=1)
    return v * cosine + swapped * sine


def normed(v, gain):
    return v * lax.rsqrt(jnp.mean(v * v, axis=-1, keepdims=True) + EPSILON) * gain


def kernel(
    K,
    T,
    lengths_h,
    inverse_h,
    hidden_h,
    gain_h,
    dq_h,
    dl_h,
    dr_h,
    qg_h,
    lg_h,
    uq_h,
    ur_h,
    ku_h,
    vu_h,
    op_h,
    lat_h,
    rope_h,
    out,
    hidden,
    gain,
    dq,
    dl,
    dr,
    qg,
    lg,
    uq,
    ur,
    ku,
    vu,
    lat,
    rope,
    rx1,
    rx2,
    rxp,
    tx3,
    rx3,
    tx4,
    rx4,
    rx6,
    spread,
    lengths,
    inverse,
    load_sem,
    s1,
    r1,
    s2,
    r2,
    sp,
    rp,
    s3,
    r3,
    s4,
    r4,
    s6,
    r6,
):
    N = K * T
    B = hidden.shape[0]
    width = hidden.shape[1] * T
    QR = dq.shape[1]
    KR = dl.shape[1]
    DR = dr.shape[0]
    Hd = uq.shape[0] // QR
    H = Hd * T
    DN = uq.shape[1]
    span = lat.shape[1]
    rows = rx3.shape[1]
    owners = tx3.shape[0]
    k = lax.axis_index("kv")
    t = lax.axis_index("tp")
    me = k * T + t
    factor = 1.0 / math.sqrt(DN + DR)

    def slot_of(kk, tt):
        first = kk * rows
        return lax.div(lax.div(first, Hd) * H + tt * Hd + lax.rem(first, Hd), rows)

    everyone_owns = owners == N

    def if_owner(kk, fn):
        if everyone_owns:
            fn()
        else:
            pl.when(kk * T * rows < B * H)(fn)

    barrier = pltpu.get_barrier_semaphore()

    def to_all(fn):
        def chip(i, carry):
            kk = k + i
            kk = jnp.where(kk >= K, kk - K, kk)
            for tt in range(T):
                fn(kk, tt)
            return carry

        lax.fori_loop(K // 2, K, chip, 0)
        lax.fori_loop(1, K // 2, chip, 0)
        for i in range(1, T):
            fn(k, lax.rem(t + i, T))

    to_all(lambda kk, tt: pl.semaphore_signal(barrier, inc=1, device_id=(kk, tt), device_id_type=MESH))

    pairs = (
        (hidden_h, hidden), (gain_h, gain), (dq_h, dq), (dl_h, dl), (dr_h, dr),
        (uq_h, uq), (ur_h, ur), (ku_h, ku), (qg_h, qg), (lg_h, lg),
        (op_h, rxp.at[t]), (lat_h, lat), (rope_h, rope), (vu_h, vu),
        (lengths_h, lengths), (inverse_h, inverse),
    )
    loads = [pltpu.make_async_copy(a, b, load_sem.at[i]) for i, (a, b) in enumerate(pairs)]
    for load in loads:
        load.start()

    spread[...] = jnp.where(
        lax.div(iota((QR, QR * Hd), 1), Hd) == iota((QR, QR * Hd), 0), 1.0, 0.0
    ).astype(BF16)
    own_rows = iota((B * H, QR * Hd), 0)
    own_mask = (lax.rem(own_rows, H) - t * Hd) == lax.rem(iota((B * H, QR * Hd), 1), Hd)

    def angles(n, per):
        row = lax.div(iota((n, DR), 0), per)
        position = jnp.zeros((n, DR), F32)
        for b in range(B):
            position = jnp.where(row == b, lengths[b].astype(F32), position)
        return sin_cos(position * inverse[...])

    for load in loads[:5]:
        load.wait()
    floats = hidden[...].astype(F32)
    scaled = (floats * gain[...]).astype(BF16)
    low = rx1.at[t]
    low[:, :QR] = dot(scaled, dq[...])
    low[:, QR : QR + KR] = dot(scaled, dl[...])
    low[:, QR + KR : QR + KR + DR] = dot_nt(scaled, dr[...])
    low[:, QR + KR + DR :] = jnp.broadcast_to(
        jnp.sum(floats * floats, axis=1, keepdims=True), (B, rx1.shape[2] - QR - KR - DR)
    )
    for load in loads[-2:]:
        load.wait()
    sine8, cosine8 = angles(B, 1)
    sine_all, cosine_all = angles(B * H, H)
    pl.semaphore_wait(barrier, N - 1)

    def swap(buffer, send, recv):
        copies = []
        for i in range(1, T):
            peer = lax.rem(t + i, T)
            copies.append(
                pltpu.make_async_remote_copy(
                    src_ref=buffer.at[t],
                    dst_ref=buffer.at[t],
                    send_sem=send.at[i],
                    recv_sem=recv.at[i],
                    device_id=(k, peer),
                    device_id_type=MESH,
                )
            )
        for copy in copies:
            copy.start()
        return copies

    copies1 = swap(rx1, s1, r1)
    for load in loads[5:-2]:
        load.wait()
    for copy in copies1:
        copy.wait()
    total = rx1[0]
    for i in range(1, T):
        total = total + rx1[i]
    inv_rms = lax.rsqrt(total[:, QR + KR + DR : QR + KR + DR + 1] / width + EPSILON)
    total = total * inv_rms
    query_normed = normed(total[:, :QR], qg[...]).astype(BF16)
    latent_new = normed(total[:, QR : QR + KR], lg[...]).astype(BF16).astype(F32)
    rope_new = turn(total[:, QR + KR : QR + KR + DR], cosine8, sine8).astype(BF16).astype(F32)

    wide = dot(query_normed, spread[...])
    wide = jnp.concatenate(
        [jnp.broadcast_to(wide[b : b + 1, :], (H, QR * Hd)) for b in range(B)], axis=0
    )
    wide = jnp.where(own_mask, wide, 0.0).astype(BF16)
    query_nope = dot(wide, uq[...]).astype(BF16)
    roped = dot_nt(query_normed, ur[...])
    roped = jnp.concatenate(
        [jnp.broadcast_to(roped[b : b + 1, :], (H, Hd * DR)) for b in range(B)], axis=0
    )
    head = lax.rem(iota((B * H, DR), 0), H) - t * Hd
    query_rope = jnp.zeros((B * H, DR), F32)
    for h in range(Hd):
        query_rope = jnp.where(head == h, roped[:, h * DR : (h + 1) * DR], query_rope)
    query_rope = turn(query_rope, cosine_all, sine_all)
    tall = jnp.where(own_mask, dot_nt(query_nope, ku[...]), 0.0).astype(BF16)
    queries = rx2.at[t]
    queries[:, :KR] = dot_nt(tall, spread[...]).astype(BF16)
    queries[:, KR : KR + DR] = query_rope.astype(BF16)
    queries[:, KR + DR :] = jnp.zeros((B * H, rx2.shape[2] - KR - DR), BF16)
    copies2 = swap(rx2, s2, r2)
    copies_p = swap(rxp, sp, rp)
    for copy in copies2:
        copy.wait()
    query = rx2[0].astype(F32)
    for i in range(1, T):
        query = query + rx2[i].astype(F32)

    offset = me * span
    lane = iota((H, span), 1) + offset
    mark = iota((H, 128), 1)
    first = me == 0
    for b in range(B):
        q = query[b * H : (b + 1) * H]
        qb = q.astype(BF16)
        usable = lane < lengths[b]
        scores = (
            dot_nt(qb[:, :KR], lat[b]) + dot(qb[:, KR : KR + DR], rope[b])
        ) * factor
        scores = jnp.where(usable, scores, -1e30)
        new_score = (
            jnp.sum(q[:, :KR] * latent_new[b : b + 1], axis=1, keepdims=True)
            + jnp.sum(q[:, KR : KR + DR] * rope_new[b : b + 1], axis=1, keepdims=True)
        ) * factor
        new_score = jnp.where(first, new_score, -1e30)
        top = jnp.maximum(jnp.max(scores, axis=1, keepdims=True), new_score)
        weights = jnp.where(usable, jnp.exp(scores - top), 0.0)
        fresh = jnp.where(first, jnp.exp(new_score - top), 0.0)
        mass = jnp.sum(weights, axis=1, keepdims=True) + fresh
        summed = dot(weights.astype(BF16), lat[b]) + fresh * latent_new[b : b + 1]
        high = top.astype(BF16).astype(F32)
        middle = (top - high).astype(BF16).astype(F32)
        small = ((top - high) - middle).astype(BF16).astype(F32)
        mass_high = mass.astype(BF16).astype(F32)
        tail = jnp.where(
            mark == 0,
            high,
            jnp.where(
                mark == 1,
                middle,
                jnp.where(mark == 2, small, jnp.where(mark == 3, mass_high, mass - mass_high)),
            ),
        )
        block = jnp.concatenate([summed, tail], axis=1).astype(BF16)
        for j in range(H // rows):
            tx3[b * (H // rows) + j] = block[j * rows : (j + 1) * rows]

    def part(kk, tt):
        return pltpu.make_async_remote_copy(
            src_ref=tx3.at[slot_of(kk, tt)],
            dst_ref=rx3.at[me],
            send_sem=s3,
            recv_sem=r3,
            device_id=(kk, tt),
            device_id_type=MESH,
        )

    to_all(lambda kk, tt: if_owner(kk, lambda: part(kk, tt).start()))

    mine = slot_of(k, t)

    def values(kk, tt):
        return pltpu.make_async_remote_copy(
            src_ref=tx4,
            dst_ref=rx4.at[mine],
            send_sem=s4,
            recv_sem=r4,
            device_id=(kk, tt),
            device_id_type=MESH,
        )

    def own():
        rx3[me] = tx3[mine]
        pltpu.make_async_copy(rx3.at[pl.ds(0, N - 1)], rx3.at[pl.ds(0, N - 1)], r3).wait()
        parts = rx3[...].astype(F32)
        tail = parts[:, :, KR : KR + 128]
        top = tail[:, :, 0:1] + tail[:, :, 1:2] + tail[:, :, 2:3]
        highest = jnp.max(top, axis=0, keepdims=True)
        scale = jnp.exp(top - highest)
        mass = jnp.sum((tail[:, :, 3:4] + tail[:, :, 4:5]) * scale, axis=0)
        attended = jnp.sum(parts[:, :, :KR] * scale, axis=0) / mass
        attended = jnp.concatenate([attended, jnp.zeros((8 - rows, KR), F32)], axis=0)
        wide = dot(attended.astype(BF16), spread[...])
        head = lax.rem(k * rows + iota((8, KR * Hd), 0), Hd)
        wide = jnp.where(head == lax.rem(iota((8, KR * Hd), 1), Hd), wide, 0.0).astype(BF16)
        value = dot(wide, vu[...])[:rows].astype(BF16)
        tx4[...] = value
        rx4[mine] = value

        to_all(lambda kk, tt: values(kk, tt).start())

    if_owner(k, own)
    for copy in copies_p:
        copy.wait()

    def arrived(n):
        pltpu.make_async_copy(rx4.at[pl.ds(0, n)], rx4.at[pl.ds(0, n)], r4).wait()

    if everyone_owns:
        arrived(owners - 1)
    else:
        owner = k * T * rows < B * H
        pl.when(owner)(lambda: arrived(owners - 1))
        pl.when(jnp.logical_not(owner))(lambda: arrived(owners))

    gathered = rx4[...].astype(F32).reshape(B, H, rx4.shape[2]).astype(BF16)
    out_cols = jnp.zeros(out.shape, F32)
    for i in range(T):
        flat = jnp.concatenate([gathered[:, i * Hd + h, :] for h in range(Hd)], axis=1)
        out_cols = out_cols + dot_nt(flat, rxp[i])
    squares = jnp.sum(out_cols * out_cols, axis=1, keepdims=True)
    diagonal = iota((B, 128), 0) == iota((B, 128), 1)
    rx6[k] = jnp.sum(jnp.where(diagonal, squares, 0.0), axis=0, keepdims=True)

    def norm_part(i):
        return pltpu.make_async_remote_copy(
            src_ref=rx6.at[k],
            dst_ref=rx6.at[k],
            send_sem=s6,
            recv_sem=r6,
            device_id=(lax.rem(k + i, K), t),
            device_id_type=MESH,
        )

    def send6(i, carry):
        norm_part(i).start()
        return carry

    lax.fori_loop(1, K, send6, 0)

    def left(buffer, n, sem):
        pltpu.make_async_copy(buffer.at[pl.ds(0, n)], buffer.at[pl.ds(0, n)], sem).wait()

    if everyone_owns:
        left(rx3, N - 1, s3)
        left(rx4, N - 1, s4)
    else:
        to_all(lambda kk, tt: if_owner(kk, lambda: part(kk, tt).wait_send()))
        if_owner(k, lambda: to_all(lambda kk, tt: values(kk, tt).wait_send()))

    pltpu.make_async_copy(rx6.at[pl.ds(0, K - 1)], rx6.at[pl.ds(0, K - 1)], r6).wait()
    total = jnp.sum(rx6[...], axis=0)
    squares = jnp.sum(
        jnp.where(diagonal, jnp.broadcast_to(total, (B, 128)), 0.0), axis=1, keepdims=True
    )
    out[...] = out_cols * lax.rsqrt(squares / width + EPSILON)
    left(rx6, K - 1, s6)


def shards(
    K, T, hidden_in, input_gain, down_query, down_latent, down_rope, query_gain, latent_gain,
    up_query, up_rope, key_up, value_up, out_proj, output_gain, latent_cache, rope_cache, lengths,
):
    B = hidden_in.shape[0]
    QR, Hd, DN = up_query.shape
    KR, DR, DV = key_up.shape[0], up_rope.shape[2], value_up.shape[2]
    H, N = Hd * T, K * T
    rows = max(1, B * Hd // K)
    owners = B * H // rows
    steps = np.arange(0, DR, 2, dtype=np.float64) / DR
    inverse = np.tile((1.0 / THETA**steps).astype(np.float32), 2)[None, :]
    flat = lambda w: w.reshape(w.shape[0] * w.shape[1], w.shape[2])
    row = lambda v: v.reshape(1, v.shape[0])
    arrays = (
        hidden_in, row(input_gain), down_query, down_latent, down_rope.T, row(query_gain),
        row(latent_gain), flat(up_query), flat(up_rope.transpose(1, 2, 0)), flat(key_up),
        flat(value_up), out_proj.T, latent_cache, rope_cache.transpose(0, 2, 1),
    )
    vm = lambda a: pltpu.VMEM(a.shape, a.dtype)
    local = [vm(a) for i, a in enumerate(arrays) if i != 11]
    low = -(-(QR + KR + DR + 1) // 128) * 128
    wide = -(-(KR + DR) // 128) * 128
    dma = pltpu.SemaphoreType.DMA
    scratch = local + [
        pltpu.VMEM((T, B, low), F32),
        pltpu.VMEM((T, B * H, wide), BF16),
        pltpu.VMEM((T,) + out_proj.shape[::-1], BF16),
        pltpu.VMEM((owners, rows, KR + 128), BF16),
        pltpu.VMEM((N, rows, KR + 128), BF16),
        pltpu.VMEM((rows, DV), BF16),
        pltpu.VMEM((owners, rows, DV), BF16),
        pltpu.VMEM((K, 1, 128), F32),
        pltpu.VMEM((QR, QR * Hd), BF16),
        pltpu.SMEM(lengths.shape, lengths.dtype),
        pltpu.VMEM(inverse.shape, F32),
        dma((len(arrays) + 2,)),
        dma((T,)), dma((T,)), dma((T,)), dma((T,)), dma((T,)), dma((T,)),
        dma, dma, dma, dma, dma, dma,
    ]
    normal = pl.pallas_call(
        functools.partial(kernel, K, T),
        out_shape=jax.ShapeDtypeStruct((B, out_proj.shape[1]), F32),
        in_specs=[pl.BlockSpec(memory_space=pl.ANY)] * (len(arrays) + 2),
        out_specs=pl.BlockSpec(memory_space=pltpu.VMEM),
        scratch_shapes=scratch,
        compiler_params=pltpu.CompilerParams(collective_id=0, has_side_effects=True),
    )(lengths, jnp.asarray(inverse), *arrays)
    return (normal * row(output_gain)).astype(BF16)


def solution(mesh):
    in_specs = (
        P(None, "tp"),
        P("tp"),
        P("tp", None),
        P("tp", None),
        P("tp", None),
        P(),
        P(),
        P(None, "tp", None),
        P(None, "tp", None),
        P(None, "tp", None),
        P(None, "tp", None),
        P("tp", "kv"),
        P("kv"),
        P(None, ("kv", "tp"), None),
        P(None, ("kv", "tp"), None),
        P(),
    )
    body = functools.partial(shards, mesh.shape["kv"], mesh.shape["tp"])
    return jax.shard_map(body, mesh=mesh, in_specs=in_specs, out_specs=P(None, "kv"), check_vma=False)
```
